32 devices in a mesh: rep: 2 (over y), fs: 4 (over z), tp: 4 (over x, core).
Axes of the slice: x: 2, y: 2, z: 4, core: 2. Of those that a mesh axis runs over, the one named last changes fastest.
Arguments:
- tokens: bfloat16 [8, 512, 2048], P(('rep', 'fs')), may hold values from -6 to 6
- first_gain: float32 [2048], replicated, may hold values from 0.1 to 1.9
- in_matrix: float32 [2048, 2048], P('fs', 'tp'), may hold values from -0.125 to 0.125
- in_scale: float32 [2048], P('tp'), may hold values from 0.5 to 2
- conv_taps: float32 [4, 2048], P(None, 'tp'), may hold values from -3 to 3
- decay_rate: float32 [2, 2048], P(None, 'tp'), may hold values from 0 to 1, as said below
- recall_maps: float32 [2, 8, 256, 256], P(None, 'tp'), may hold values from -0.375 to 0.375
- admit_maps: float32 [2, 8, 256, 256], P(None, 'tp'), may hold values from -0.375 to 0.375
- out_matrix: float32 [2048, 2048], P('fs', 'tp'), may hold values from -0.125 to 0.125
- out_scale: float32 [2048], P('fs'), may hold values from 0.5 to 2
- second_gain: float32 [2048], replicated, may hold values from 0.1 to 1.9
- up_matrix: float32 [2048, 4096], P('fs', 'tp'), may hold values from -0.125 to 0.125
- up_scale: float32 [4096], P('tp'), may hold values from 0.5 to 2
- down_matrix: float32 [2048, 4096], P('fs', 'tp'), may hold values from -0.09375 to 0.09375
- down_scale: float32 [2048], P('fs'), may hold values from 0.5 to 2
Outputs:
- layer_out: bfloat16 [8, 512, 2048], P(('rep', 'fs'))
The draws below stay inside these ranges and needn't reach their ends.
Inputs may be any that keep to these rules, and one draw needn't show every extreme that they name: `decay_rate`: positive per-step decay rates.
All inputs are finite; a program needn't handle non-finite values.
Results may differ from the reference program's by a relative error of at most 0.024.
Values may be sent and summed in bfloat16 or wider, within the bound.
No kernel may reach another device: no remote copies, remote signals or barrier semaphores. Data moves between devices by JAX's collectives and lax.ppermute only.
A program may use at most 64 MiB of HBM per device.

```python
import math
import jax
import jax.numpy as jnp
from jax import lax

D = 2048
BLOCK = 256
BLOCKS = 8
FF = 4096
TAPS = 4
LEN = 512
REC_WIDTH = 2048
SEQS = 8
N_TP = 4


def draw_decay_rate(key, part):
    pick_key, slow_key, fast_key = jax.random.split(jax.random.fold_in(key, 17), 3)
    shape = (2, REC_WIDTH)
    slow_share = 0.5
    slow_pick = jax.random.bernoulli(pick_key, slow_share, shape)
    slow_rate = jnp.exp(jax.random.uniform(slow_key, shape, jnp.float32, math.log(0.05), math.log(0.5))) / LEN
    fast_rate = jnp.exp(jax.random.uniform(fast_key, shape, jnp.float32, math.log(0.005), math.log(0.02)))
    return jnp.where(slow_pick, slow_rate, fast_rate).astype(jnp.float32)


def level_of(key, extent, cuts, least, top_value):
    factor_of, own = 1.0, jax.random.fold_in(key, 6)
    for dim, blocks in cuts:
        heights = jnp.exp(jax.random.uniform(jax.random.fold_in(own, dim), (blocks,), jnp.float32, least / len(cuts), top_value / len(cuts)))
        factor_of = factor_of * jnp.repeat(heights, extent[dim] // blocks).reshape([-1 if axis == dim else 1 for axis in range(len(extent))])
    return factor_of


def bell_draw(rng, dims, deviation, reach, pieces=(), dtype=jnp.bfloat16):
    level = level_of(rng, dims, pieces, -0.22, 0.18) if pieces else 1.0
    entries = jax.random.normal(rng, dims, jnp.float32) * deviation * level
    return jnp.minimum(jnp.maximum(entries, -reach), reach).astype(dtype)


def setup_inputs(seed: int = 0) -> dict:
    seeds = jax.random.split(jax.random.key(seed), 16)
    return {
        "tokens": bell_draw(seeds[0], (SEQS, LEN, D), 1.0, 6.0, ((0, 8),)),
        "first_gain": jnp.clip(1.0 + 0.18 * jax.random.normal(seeds[1], (D,), jnp.float32), 0.1, 1.9),
        "in_matrix": bell_draw(seeds[2], (D, REC_WIDTH), D ** -0.5, 0.125, ((0, 4), (1, 4)), jnp.float32),
        "in_scale": jnp.clip(jnp.exp(math.log(2.0) - 1.3862944 * jax.random.uniform(seeds[3], (REC_WIDTH,), jnp.float32) ** level_of(seeds[3], (REC_WIDTH,), ((0, 4),), -0.2, 0.2)), 0.5, 2.0),
        "conv_taps": bell_draw(seeds[4], (TAPS, REC_WIDTH), TAPS ** -0.5, 3.0, ((1, 4),), jnp.float32),
        "decay_rate": draw_decay_rate(jax.random.fold_in(seeds[15], 71), 0),
        "recall_maps": bell_draw(seeds[6], (2, BLOCKS, BLOCK, BLOCK), BLOCK ** -0.5, 0.375, ((1, 4),), jnp.float32),
        "admit_maps": bell_draw(seeds[7], (2, BLOCKS, BLOCK, BLOCK), BLOCK ** -0.5, 0.375, ((1, 4),), jnp.float32),
        "out_matrix": bell_draw(seeds[8], (D, REC_WIDTH), REC_WIDTH ** -0.5, 0.125, ((0, 4), (1, 4)), jnp.float32),
        "out_scale": jnp.clip(jnp.exp(math.log(2.0) - 1.3862944 * jax.random.uniform(seeds[9], (D,), jnp.float32) ** level_of(seeds[9], (D,), ((0, 4),), -0.2, 0.2)), 0.5, 2.0),
        "second_gain": jnp.clip(1.0 + 0.18 * jax.random.normal(seeds[10], (D,), jnp.float32), 0.1, 1.9),
        "up_matrix": bell_draw(seeds[11], (D, FF), D ** -0.5, 0.125, ((0, 4), (1, 4)), jnp.float32),
        "up_scale": jnp.clip(jnp.exp(math.log(2.0) - 1.3862944 * jax.random.uniform(seeds[12], (FF,), jnp.float32) ** level_of(seeds[12], (FF,), ((0, 4),), -0.2, 0.2)), 0.5, 2.0),
        "down_matrix": bell_draw(seeds[13], (D, FF), FF ** -0.5, 0.09375, ((0, 4), (1, 4)), jnp.float32),
        "down_scale": jnp.clip(jnp.exp(math.log(2.0) - 1.3862944 * jax.random.uniform(seeds[14], (D,), jnp.float32) ** level_of(seeds[14], (D,), ((0, 4),), -0.2, 0.2)), 0.5, 2.0),
    }


EPSILON = 1e-06
RATE_GAIN = 8.0

def normalize(stream, gain):
    return stream * lax.rsqrt(lax.optimization_barrier(jnp.mean(stream * stream, axis=-1, keepdims=True)) + EPSILON) * gain

def convolve(values, taps):
    length = values.shape[0]
    count = taps.shape[0]
    padded = jnp.pad(values, ((count // 2, count - 1 - count // 2), (0, 0)))
    total = taps[0] * padded[0:length]
    for offset in range(1, count):
        total = total + taps[offset] * padded[offset:offset + length]
    return total

def block_map(values, maps):
    length = values.shape[0]
    count, width = (maps.shape[0], maps.shape[1])
    grouped = values.reshape(length, count, width)
    mapped = jnp.einsum('lnj,njk->lnk', grouped, maps, precision=lax.Precision.HIGHEST)
    return mapped.reshape(length, count * width)

def combine_steps(earlier, later):
    return (earlier[0] * later[0], later[0] * earlier[1] + later[1])

def one_direction(values, rate, recall_map, admit_map):
    recall = jax.nn.sigmoid(block_map(values, recall_map))
    admit = jax.nn.sigmoid(block_map(values, admit_map))
    log_decay = -RATE_GAIN * recall * rate
    decay = jnp.exp(log_decay)
    drive = jnp.sqrt(-jnp.expm1(2.0 * log_decay)) * admit * values
    carried = lax.associative_scan(combine_steps, (decay, drive), axis=0)
    return carried[1]

def recurrence(values, rates, recall_maps, admit_maps):
    forward = one_direction(values, rates[0], recall_maps[0], admit_maps[0])
    backward = one_direction(values[::-1], rates[1], recall_maps[1], admit_maps[1])[::-1]
    return forward + backward

def block_sum(values, matrix):
    length, width = values.shape
    model = matrix.shape[0]
    split_values = values.astype(jnp.float32).reshape(length, N_TP, width // N_TP)
    split_matrix = matrix.astype(jnp.float32).reshape(model, N_TP, width // N_TP)
    parts = jnp.einsum('lte,dte->tld', split_values, split_matrix, precision=lax.Precision.HIGHEST)
    rounded = lax.optimization_barrier(parts.astype(jnp.bfloat16))
    return lax.optimization_barrier(jnp.sum(rounded.astype(jnp.float32), axis=0))

def reference(tokens, first_gain, in_matrix, in_scale, conv_taps, decay_rate, recall_maps, admit_maps, out_matrix, out_scale, second_gain, up_matrix, up_scale, down_matrix, down_scale):
    in_cols = in_matrix.astype(jnp.bfloat16)
    out_rows = out_matrix.astype(jnp.bfloat16)
    up_cols = up_matrix.astype(jnp.bfloat16)
    down_rows = down_matrix.astype(jnp.bfloat16)
    in_factor = in_scale.astype(jnp.bfloat16)
    out_factor = out_scale.astype(jnp.bfloat16)
    up_factor = up_scale.astype(jnp.bfloat16)
    down_factor = down_scale.astype(jnp.bfloat16)

    def one_sequence(sequence):
        stream = sequence.astype(jnp.float32)
        normed = normalize(stream, first_gain).astype(jnp.bfloat16)
        before = (jnp.dot(normed, in_cols, preferred_element_type=jnp.float32) * in_factor).astype(jnp.bfloat16)
        conv_out = convolve(before.astype(jnp.float32), conv_taps)
        mixed = recurrence(conv_out, decay_rate, recall_maps, admit_maps).astype(jnp.bfloat16)
        middle = stream + out_factor * block_sum(mixed, out_rows)
        second_normed = normalize(middle, second_gain).astype(jnp.bfloat16)
        raised = jnp.dot(second_normed, up_cols, preferred_element_type=jnp.float32) * up_factor
        active = jnp.square(jax.nn.relu(raised)).astype(jnp.bfloat16)
        return (middle + down_factor * block_sum(active, down_rows)).astype(jnp.bfloat16)
    return lax.map(one_sequence, tokens)
```

```python
import jax
import jax.numpy as jnp
from jax import lax
from jax.experimental import pallas as pl
from jax.experimental.pallas import tpu as pltpu
from jax.sharding import PartitionSpec as P

EPSILON = 1e-06
RATE_GAIN = 8.0


def normalize(stream, gain):
    return stream * lax.rsqrt(jnp.mean(stream * stream, axis=-1, keepdims=True) + EPSILON) * gain


SEGMENTS = 8
LANES = 128


def one_minus_exp(y):
    series = -y * (1.0 + y * (1.0 / 2) * (1.0 + y * (1.0 / 3) * (1.0 + y * 0.25 * (1.0 + y * 0.2))))
    return jnp.where(y > -0.25, series, 1.0 - jnp.exp(y))


def sigmoid(x):
    return 1.0 / (1.0 + jnp.exp(-x))


def recurrence_kernel(before, taps, rates, recall_maps, admit_maps, mixed, padded, hi, lo, decay, drive, states):
    length, width = before.shape
    count = taps.shape[0]
    front = 8
    tiles = width // LANES
    padded[pl.ds(0, front), :] = jnp.zeros((front, width), jnp.float32)
    padded[pl.ds(front, length), :] = before[...].astype(jnp.float32)
    padded[pl.ds(front + length, 8), :] = jnp.zeros((8, width), jnp.float32)
    for slot in range(4):
        source = (recall_maps, admit_maps)[slot % 2]
        values = source[slot // 2, 0]
        top = values.astype(jnp.bfloat16)
        hi[:, slot * width : (slot + 1) * width] = top
        lo[:, slot * width : (slot + 1) * width] = (values - top.astype(jnp.float32)).astype(jnp.bfloat16)
    rows = min(128, length)
    for start in range(0, length, rows):
        total = taps[0:1, :] * padded[pl.ds(front + start - count // 2, rows), :]
        for offset in range(1, count):
            total = total + taps[offset : offset + 1, :] * padded[pl.ds(front + start + offset - count // 2, rows), :]
        top = total.astype(jnp.bfloat16)
        rest = (total - top.astype(jnp.float32)).astype(jnp.bfloat16)
        for direction in range(2):
            span = slice(direction * 2 * width, (direction + 1) * 2 * width)
            gates = (
                jnp.dot(top, hi[:, span], preferred_element_type=jnp.float32)
                + jnp.dot(rest, hi[:, span], preferred_element_type=jnp.float32)
                + jnp.dot(top, lo[:, span], preferred_element_type=jnp.float32)
            )
            recall = sigmoid(gates[:, :width])
            admit = sigmoid(gates[:, width:])
            log_decay = (-RATE_GAIN * rates[direction : direction + 1, :]) * recall
            step_decay = jnp.exp(log_decay)
            step_drive = jnp.sqrt(one_minus_exp(2.0 * log_decay)) * admit * total
            for tile in range(tiles):
                lanes = slice(tile * LANES, (tile + 1) * LANES)
                decay[direction * tiles + tile, pl.ds(start, rows), :] = step_decay[:, lanes]
                drive[direction * tiles + tile, pl.ds(start, rows), :] = step_drive[:, lanes]
    step = length // SEGMENTS
    zero = jnp.zeros((SEGMENTS, LANES), jnp.float32)
    one = jnp.ones((SEGMENTS, LANES), jnp.float32)

    def picked(ref, lane, i):
        at = i if lane < tiles else step - 1 - i
        return ref[lane, pl.ds(at, SEGMENTS, stride=step), :]

    def first_pass(i, carry):
        after = []
        for lane, (state, product) in enumerate(carry):
            a = picked(decay, lane, i)
            after.append((a * state + picked(drive, lane, i), a * product))
        return tuple(after)

    ends = lax.fori_loop(0, step, first_pass, ((zero, one),) * (2 * tiles), unroll=8)
    begins = []
    for lane, (state, product) in enumerate(ends):
        row = zero[0:1]
        rows_of = [row]
        order = range(SEGMENTS - 1) if lane < tiles else range(SEGMENTS - 1, 0, -1)
        for s in order:
            row = state[s : s + 1] + product[s : s + 1] * row
            rows_of.append(row)
        begins.append(jnp.concatenate(rows_of if lane < tiles else rows_of[::-1], axis=0))

    def second_pass(i, carry):
        after = []
        for lane, state in enumerate(carry):
            state = picked(decay, lane, i) * state + picked(drive, lane, i)
            at = i if lane < tiles else step - 1 - i
            states[lane, pl.ds(at, SEGMENTS, stride=step), :] = state
            after.append(state)
        return tuple(after)

    lax.fori_loop(0, step, second_pass, tuple(begins), unroll=8)
    for tile in range(tiles):
        mixed[:, tile * LANES : (tile + 1) * LANES] = (states[tile] + states[tiles + tile]).astype(jnp.bfloat16)


def recurrence(before, taps, rates, recall_maps, admit_maps):
    length, channels = before.shape
    groups, width = recall_maps.shape[1:3]
    column = lambda g: (0, g)
    return pl.pallas_call(
        recurrence_kernel,
        grid=(groups,),
        in_specs=[
            pl.BlockSpec((length, width), column),
            pl.BlockSpec((taps.shape[0], width), column),
            pl.BlockSpec((2, width), column),
            pl.BlockSpec((2, 1, width, width), lambda g: (0, g, 0, 0)),
            pl.BlockSpec((2, 1, width, width), lambda g: (0, g, 0, 0)),
        ],
        out_specs=pl.BlockSpec((length, width), column),
        out_shape=jax.ShapeDtypeStruct((length, channels), jnp.bfloat16),
        scratch_shapes=[
            pltpu.VMEM((length + 16, width), jnp.float32),
            pltpu.VMEM((width, 4 * width), jnp.bfloat16),
            pltpu.VMEM((width, 4 * width), jnp.bfloat16),
            pltpu.VMEM((2 * width // LANES, length, LANES), jnp.float32),
            pltpu.VMEM((2 * width // LANES, length, LANES), jnp.float32),
            pltpu.VMEM((2 * width // LANES, length, LANES), jnp.float32),
        ],
        compiler_params=pltpu.CompilerParams(dimension_semantics=("arbitrary",)),
        name="recurrence",
    )(before, taps, rates, recall_maps, admit_maps)


def contract_last(left, right):
    return lax.dot_general(
        left, right, (((1,), (1,)), ((), ())), preferred_element_type=jnp.float32
    )


def body(
    tokens,
    first_gain,
    in_matrix,
    in_scale,
    conv_taps,
    decay_rate,
    recall_maps,
    admit_maps,
    out_matrix,
    out_scale,
    second_gain,
    up_matrix,
    up_scale,
    down_matrix,
    down_scale,
):
    stream = tokens.reshape(tokens.shape[1], tokens.shape[2]).astype(jnp.float32)
    in_cols, out_rows, out_factor, down_factor = (
        lax.all_gather(in_matrix.astype(jnp.bfloat16), "fs", axis=0, tiled=True),
        lax.all_gather(out_matrix.astype(jnp.bfloat16), "fs", axis=0, tiled=True),
        lax.all_gather(out_scale.astype(jnp.bfloat16), "fs", axis=0, tiled=True),
        lax.all_gather(down_scale.astype(jnp.bfloat16), "fs", axis=0, tiled=True),
    )
    normed = normalize(stream, first_gain).astype(jnp.bfloat16)
    before = (
        jnp.dot(normed, in_cols, preferred_element_type=jnp.float32) * in_scale.astype(jnp.bfloat16)
    ).astype(jnp.bfloat16)
    mixed = recurrence(before, conv_taps, decay_rate, recall_maps, admit_maps)
    partial_value = contract_last(mixed, out_rows)
    middle = stream + out_factor * lax.psum(partial_value.astype(jnp.bfloat16), "tp").astype(
        jnp.float32
    )
    second_normed = normalize(middle, second_gain).astype(jnp.bfloat16)
    raised = jnp.dot(
        second_normed,
        lax.all_gather(up_matrix.astype(jnp.bfloat16), "fs", axis=0, tiled=True),
        preferred_element_type=jnp.float32,
    )
    active = jnp.square(jax.nn.relu(raised * up_scale.astype(jnp.bfloat16))).astype(jnp.bfloat16)
    lowered = contract_last(
        active, lax.all_gather(down_matrix.astype(jnp.bfloat16), "fs", axis=0, tiled=True)
    )
    result = (
        middle + down_factor * lax.psum(lowered.astype(jnp.bfloat16), "tp").astype(jnp.float32)
    ).astype(jnp.bfloat16)
    return result.reshape(tokens.shape)


def solution(mesh):
    placed = (
        P(("rep", "fs"), None, None),
        P(),
        P("fs", "tp"),
        P("tp"),
        P(None, "tp"),
        P(None, "tp"),
        P(None, "tp", None, None),
        P(None, "tp", None, None),
        P("fs", "tp"),
        P("fs"),
        P(),
        P("fs", "tp"),
        P("tp"),
        P("fs", "tp"),
        P("fs"),
    )
    return jax.shard_map(
        body, mesh=mesh, in_specs=placed, out_specs=P(("rep", "fs"), None, None), check_vma=False
    )
```

```python
from functools import partial

import jax
import jax.numpy as jnp
from jax import lax
from jax.experimental import pallas as pl
from jax.experimental.pallas import tpu as pltpu
from jax.sharding import PartitionSpec as P

EPSILON = 1e-06
RATE_GAIN = 8.0


def normalize(stream, gain):
    return stream * lax.rsqrt(jnp.mean(stream * stream, axis=-1, keepdims=True) + EPSILON) * gain


SEGMENTS = 8
LANES = 128
FRONT = 8


def one_minus_exp(y):
    series = -y * (1.0 + y * (1.0 / 2) * (1.0 + y * (1.0 / 3) * (1.0 + y * 0.25 * (1.0 + y * 0.2))))
    return jnp.where(y > -0.25, series, 1.0 - jnp.exp(y))


def sigmoid(x):
    return 1.0 / (1.0 + jnp.exp(-x))


def recurrence_kernel(before, taps, rates, recall_maps, admit_maps, mixed, padded, *scratch):
    padded[pl.ds(FRONT, before.shape[0]), :] = before[...].astype(jnp.float32)
    recur(taps, rates, recall_maps, admit_maps, mixed, padded, *scratch)


def recur(taps, rates, recall_maps, admit_maps, mixed, padded, hi, lo, decay, drive, states):
    length, width = mixed.shape
    count = taps.shape[0]
    front = FRONT
    tiles = width // LANES
    padded[pl.ds(0, front), :] = jnp.zeros((front, width), jnp.float32)
    padded[pl.ds(front + length, 8), :] = jnp.zeros((8, width), jnp.float32)
    for slot in range(4):
        source = (recall_maps, admit_maps)[slot % 2]
        values = source[slot // 2, 0]
        top = values.astype(jnp.bfloat16)
        hi[:, slot * width : (slot + 1) * width] = top
        lo[:, slot * width : (slot + 1) * width] = (values - top.astype(jnp.float32)).astype(jnp.bfloat16)
    rows = min(128, length)
    for start in range(0, length, rows):
        total = taps[0:1, :] * padded[pl.ds(front + start - count // 2, rows), :]
        for offset in range(1, count):
            total = total + taps[offset : offset + 1, :] * padded[pl.ds(front + start + offset - count // 2, rows), :]
        top = total.astype(jnp.bfloat16)
        rest = (total - top.astype(jnp.float32)).astype(jnp.bfloat16)
        for direction in range(2):
            span = slice(direction * 2 * width, (direction + 1) * 2 * width)
            gates = (
                jnp.dot(top, hi[:, span], preferred_element_type=jnp.float32)
                + jnp.dot(rest, hi[:, span], preferred_element_type=jnp.float32)
                + jnp.dot(top, lo[:, span], preferred_element_type=jnp.float32)
            )
            recall = sigmoid(gates[:, :width])
            admit = sigmoid(gates[:, width:])
            log_decay = (-RATE_GAIN * rates[direction : direction + 1, :]) * recall
            step_decay = jnp.exp(log_decay)
            step_drive = jnp.sqrt(one_minus_exp(2.0 * log_decay)) * admit * total
            for tile in range(tiles):
                lanes = slice(tile * LANES, (tile + 1) * LANES)
                decay[direction * tiles + tile, pl.ds(start, rows), :] = step_decay[:, lanes]
                drive[direction * tiles + tile, pl.ds(start, rows), :] = step_drive[:, lanes]
    step = length // SEGMENTS
    zero = jnp.zeros((SEGMENTS, LANES), jnp.float32)
    one = jnp.ones((SEGMENTS, LANES), jnp.float32)

    def picked(ref, lane, i):
        at = i if lane < tiles else step - 1 - i
        return ref[lane, pl.ds(at, SEGMENTS, stride=step), :]

    def first_pass(i, carry):
        after = []
        for lane, (state, product) in enumerate(carry):
            a = picked(decay, lane, i)
            after.append((a * state + picked(drive, lane, i), a * product))
        return tuple(after)

    ends = lax.fori_loop(0, step, first_pass, ((zero, one),) * (2 * tiles), unroll=8)
    begins = []
    for lane, (state, product) in enumerate(ends):
        row = zero[0:1]
        rows_of = [row]
        order = range(SEGMENTS - 1) if lane < tiles else range(SEGMENTS - 1, 0, -1)
        for s in order:
            row = state[s : s + 1] + product[s : s + 1] * row
            rows_of.append(row)
        begins.append(jnp.concatenate(rows_of if lane < tiles else rows_of[::-1], axis=0))

    def second_pass(i, carry):
        after = []
        for lane, state in enumerate(carry):
            state = picked(decay, lane, i) * state + picked(drive, lane, i)
            at = i if lane < tiles else step - 1 - i
            states[lane, pl.ds(at, SEGMENTS, stride=step), :] = state
            after.append(state)
        return tuple(after)

    lax.fori_loop(0, step, second_pass, tuple(begins), unroll=8)
    for tile in range(tiles):
        mixed[:, tile * LANES : (tile + 1) * LANES] = (states[tile] + states[tiles + tile]).astype(jnp.bfloat16)


def recurrence_scratch(length, width):
    return [
        pltpu.VMEM((length + 2 * FRONT, width), jnp.float32),
        pltpu.VMEM((width, 4 * width), jnp.bfloat16),
        pltpu.VMEM((width, 4 * width), jnp.bfloat16),
        pltpu.VMEM((2 * width // LANES, length, LANES), jnp.float32),
        pltpu.VMEM((2 * width // LANES, length, LANES), jnp.float32),
        pltpu.VMEM((2 * width // LANES, length, LANES), jnp.float32),
    ]


def recurrence(before, taps, rates, recall_maps, admit_maps):
    length, channels = before.shape
    groups, width = recall_maps.shape[1:3]
    column = lambda g: (0, g)
    return pl.pallas_call(
        recurrence_kernel,
        grid=(groups,),
        in_specs=[
            pl.BlockSpec((length, width), column),
            pl.BlockSpec((taps.shape[0], width), column),
            pl.BlockSpec((2, width), column),
            pl.BlockSpec((2, 1, width, width), lambda g: (0, g, 0, 0)),
            pl.BlockSpec((2, 1, width, width), lambda g: (0, g, 0, 0)),
        ],
        out_specs=pl.BlockSpec((length, width), column),
        out_shape=jax.ShapeDtypeStruct((length, channels), jnp.bfloat16),
        scratch_shapes=recurrence_scratch(length, width),
        compiler_params=pltpu.CompilerParams(dimension_semantics=("arbitrary",)),
        name="recurrence",
    )(before, taps, rates, recall_maps, admit_maps)


def contract_last(left, right):
    return lax.dot_general(
        left, right, (((1,), (1,)), ((), ())), preferred_element_type=jnp.float32
    )


def plain_body(
    tokens,
    first_gain,
    in_matrix,
    in_scale,
    conv_taps,
    decay_rate,
    recall_maps,
    admit_maps,
    out_matrix,
    out_scale,
    second_gain,
    up_matrix,
    up_scale,
    down_matrix,
    down_scale,
):
    stream = tokens.reshape(tokens.shape[1], tokens.shape[2]).astype(jnp.float32)
    in_cols, out_rows, out_factor, down_factor = (
        lax.all_gather(in_matrix.astype(jnp.bfloat16), "fs", axis=0, tiled=True),
        lax.all_gather(out_matrix.astype(jnp.bfloat16), "fs", axis=0, tiled=True),
        lax.all_gather(out_scale.astype(jnp.bfloat16), "fs", axis=0, tiled=True),
        lax.all_gather(down_scale.astype(jnp.bfloat16), "fs", axis=0, tiled=True),
    )
    normed = normalize(stream, first_gain).astype(jnp.bfloat16)
    before = (
        jnp.dot(normed, in_cols, preferred_element_type=jnp.float32) * in_scale.astype(jnp.bfloat16)
    ).astype(jnp.bfloat16)
    mixed = recurrence(before, conv_taps, decay_rate, recall_maps, admit_maps)
    partial_value = contract_last(mixed, out_rows)
    middle = stream + out_factor * lax.psum(partial_value.astype(jnp.bfloat16), "tp").astype(
        jnp.float32
    )
    second_normed = normalize(middle, second_gain).astype(jnp.bfloat16)
    raised = jnp.dot(
        second_normed,
        lax.all_gather(up_matrix.astype(jnp.bfloat16), "fs", axis=0, tiled=True),
        preferred_element_type=jnp.float32,
    )
    active = jnp.square(jax.nn.relu(raised * up_scale.astype(jnp.bfloat16))).astype(jnp.bfloat16)
    lowered = contract_last(
        active, lax.all_gather(down_matrix.astype(jnp.bfloat16), "fs", axis=0, tiled=True)
    )
    result = (
        middle + down_factor * lax.psum(lowered.astype(jnp.bfloat16), "tp").astype(jnp.float32)
    ).astype(jnp.bfloat16)
    return result.reshape(tokens.shape)


def whole(shape):
    return pl.BlockSpec(shape, lambda *_: (0,) * len(shape))


def scalars():
    return pl.BlockSpec(memory_space=pltpu.SMEM)


def reorder_kernel(places, tokens, gain, normed, stream, *, chunk):
    rows, features = tokens.shape
    values = tokens[...].astype(jnp.float32)
    inverse = lax.rsqrt(jnp.sum(values * values, axis=-1, keepdims=True) * (1.0 / features) + EPSILON)
    for slot in range(features // chunk):
        here = pl.ds(pl.multiple_of(places[slot] * chunk, chunk), chunk)
        piece = tokens[:, here]
        stream[:, slot * chunk : (slot + 1) * chunk] = piece
        normed[:, slot * chunk : (slot + 1) * chunk] = (
            piece.astype(jnp.float32) * inverse * gain[:, here]
        ).astype(jnp.bfloat16)


def reorder(places, tokens, gain, chunk):
    length, features = tokens.shape
    rows = min(128, length)
    by_rows = pl.BlockSpec((rows, features), lambda i: (i, 0))
    return pl.pallas_call(
        partial(reorder_kernel, chunk=chunk),
        grid=(length // rows,),
        in_specs=[scalars(), by_rows, whole((1, features))],
        out_specs=[by_rows, by_rows],
        out_shape=[jax.ShapeDtypeStruct((length, features), jnp.bfloat16)] * 2,
        name="reorder",
    )(places, tokens, gain.reshape(1, features))


def mixer_kernel(normed, scale, taps, rates, recall_maps, admit_maps, *rest, pieces):
    weights, mixed, padded = rest[:pieces], rest[pieces], rest[pieces + 1]
    length = mixed.shape[0]
    chunk = weights[0].shape[0]
    rows = min(256, length)
    factor = scale[...].astype(jnp.bfloat16).astype(jnp.float32)
    for start in range(0, length, rows):
        total = None
        for slot, weight in enumerate(weights):
            part = jnp.dot(
                normed[start : start + rows, slot * chunk : (slot + 1) * chunk],
                weight[...],
                preferred_element_type=jnp.float32,
            )
            total = part if total is None else total + part
        padded[pl.ds(FRONT + start, rows), :] = (total * factor).astype(jnp.bfloat16).astype(jnp.float32)
    recur(taps, rates, recall_maps, admit_maps, mixed, padded, *rest[pieces + 2 :])


def mixer(normed, weights, scale, taps, rates, recall_maps, admit_maps):
    length, features = normed.shape
    groups, width = recall_maps.shape[1:3]
    channels = groups * width
    column = lambda g: (0, g)
    return pl.pallas_call(
        partial(mixer_kernel, pieces=len(weights)),
        grid=(groups,),
        in_specs=[
            whole((length, features)),
            pl.BlockSpec((1, width), column),
            pl.BlockSpec((taps.shape[0], width), column),
            pl.BlockSpec((2, width), column),
            pl.BlockSpec((2, 1, width, width), lambda g: (0, g, 0, 0)),
            pl.BlockSpec((2, 1, width, width), lambda g: (0, g, 0, 0)),
        ]
        + [pl.BlockSpec((weight.shape[0], width), column) for weight in weights],
        out_specs=pl.BlockSpec((length, width), column),
        out_shape=jax.ShapeDtypeStruct((length, channels), jnp.bfloat16),
        scratch_shapes=recurrence_scratch(length, width),
        cost_estimate=pl.CostEstimate(flops=8 * 10**9, bytes_accessed=8 * 2**20, transcendentals=0),
        name="mixer",
    )(normed, scale.reshape(1, channels), taps, rates, recall_maps, admit_maps, *weights)


def project_kernel(core, values, *rest, pieces, chunk):
    weights, kept, sent = rest[:pieces], rest[pieces], rest[pieces + 1]
    first = core[0] == 0
    for block in range(pieces // 2):
        parts = [
            lax.dot_general(
                values[...], weights[2 * block + side][0:chunk, :], (((1,), (1,)), ((), ())), preferred_element_type=jnp.float32
            )
            for side in range(2)
        ]
        span = slice(block * chunk, (block + 1) * chunk)
        kept[:, span] = jnp.where(first, parts[0], parts[1]).astype(jnp.bfloat16)
        sent[:, span] = jnp.where(first, parts[1], parts[0]).astype(jnp.bfloat16)


def project(core, values, weights, chunk):
    length, inner = values.shape
    rows = min(256, length)
    features = len(weights) // 2 * chunk
    by_rows = pl.BlockSpec((rows, features), lambda i: (i, 0))
    return pl.pallas_call(
        partial(project_kernel, pieces=len(weights), chunk=chunk),
        grid=(length // rows,),
        in_specs=[scalars(), pl.BlockSpec((rows, inner), lambda i: (i, 0))] + [whole(weight.shape) for weight in weights],
        out_specs=[by_rows, by_rows],
        out_shape=[jax.ShapeDtypeStruct((length, features), jnp.bfloat16)] * 2,
        cost_estimate=pl.CostEstimate(flops=4 * length * inner * features, bytes_accessed=4 * 2**20, transcendentals=0),
        name="project",
    )(core, values, *weights)


def expand_kernel(places, core, stream, own_mix, peer_mix, scales, gain, up_scale, *rest, pieces):
    weights, active, middle, work = rest[:pieces], rest[pieces], rest[pieces + 1], rest[pieces + 2]
    rows, features = stream.shape
    chunk = features // pieces
    first = core[0] == 0
    squares = None
    for slot in range(pieces):
        span = slice(slot * chunk, (slot + 1) * chunk)
        block = slice(slot // 2 * chunk, (slot // 2 + 1) * chunk)
        near, far = (own_mix, peer_mix) if slot % 2 == 0 else (peer_mix, own_mix)
        mix = jnp.where(first, near[:, block].astype(jnp.float32), far[:, block].astype(jnp.float32))
        piece = stream[:, span].astype(jnp.float32) + scales[:, span] * mix
        work[:, span] = piece
        part = jnp.sum(piece * piece, axis=-1, keepdims=True)
        squares = part if squares is None else squares + part
    inverse = lax.rsqrt(squares * (1.0 / features) + EPSILON)
    total = None
    for slot in range(pieces):
        span = slice(slot * chunk, (slot + 1) * chunk)
        here = pl.ds(pl.multiple_of(places[slot] * chunk, chunk), chunk)
        second = (work[:, span] * inverse * gain[:, here]).astype(jnp.bfloat16)
        part = jnp.dot(second, weights[slot][...], preferred_element_type=jnp.float32)
        total = part if total is None else total + part
    for block in range(pieces // 2):
        span = slice(block * chunk, (block + 1) * chunk)
        low = work[:, 2 * block * chunk : (2 * block + 1) * chunk]
        high = work[:, (2 * block + 1) * chunk : (2 * block + 2) * chunk]
        middle[:, span] = jnp.where(first, low, high)
    raised = jnp.maximum(total * up_scale[...].astype(jnp.bfloat16).astype(jnp.float32), 0.0)
    active[...] = (raised * raised).astype(jnp.bfloat16)


def expand(places, core, stream, own_mix, peer_mix, scales, gain, up_scale, weights):
    length, features = stream.shape
    hidden = weights[0].shape[1]
    rows = min(128, length)
    half = features // 2
    by_rows = lambda wide: pl.BlockSpec((rows, wide), lambda i: (i, 0))
    return pl.pallas_call(
        partial(expand_kernel, pieces=len(weights)),
        grid=(length // rows,),
        in_specs=[
            scalars(),
            scalars(),
            by_rows(features),
            by_rows(half),
            by_rows(half),
            whole((1, features)),
            whole((1, features)),
            whole((1, hidden)),
        ]
        + [whole(weight.shape) for weight in weights],
        out_specs=[by_rows(hidden), by_rows(half)],
        out_shape=[
            jax.ShapeDtypeStruct((length, hidden), jnp.bfloat16),
            jax.ShapeDtypeStruct((length, half), jnp.float32),
        ],
        scratch_shapes=[pltpu.VMEM((rows, features), jnp.float32)],
        cost_estimate=pl.CostEstimate(flops=2 * length * features * hidden, bytes_accessed=8 * 2**20, transcendentals=0),
        name="expand",
    )(places, core, stream, own_mix, peer_mix, scales, gain.reshape(1, features), up_scale.reshape(1, hidden), *weights)


def place_kernel(places, core, *rest, blocks):
    own, peer, result = rest[:blocks], rest[blocks : 2 * blocks], rest[2 * blocks]
    chunk = own[0].shape[1]
    first = core[0] == 0
    for block in range(blocks):
        for side in range(2):
            near, far = (own, peer) if side == 0 else (peer, own)
            here = pl.ds(pl.multiple_of(places[2 * block + side] * chunk, chunk), chunk)
            result[:, here] = jnp.where(first, near[block][...], far[block][...])


def place(places, core, own, peer):
    length, chunk = own[0].shape
    blocks = len(own)
    features = 2 * blocks * chunk
    rows = min(256, length)
    piece = pl.BlockSpec((rows, chunk), lambda i: (i, 0))
    return pl.pallas_call(
        partial(place_kernel, blocks=blocks),
        grid=(length // rows,),
        in_specs=[scalars(), scalars()] + [piece] * (2 * blocks),
        out_specs=pl.BlockSpec((rows, features), lambda i: (i, 0)),
        out_shape=jax.ShapeDtypeStruct((length, features), jnp.bfloat16),
        name="place",
    )(places, core, *own, *peer)


def ring_order(size):
    return list(range(0, size, 2)) + list(range(size - 1 - size % 2, 0, -2))


def ring_body(
    tokens,
    first_gain,
    in_matrix,
    in_scale,
    conv_taps,
    decay_rate,
    recall_maps,
    admit_maps,
    out_matrix,
    out_scale,
    second_gain,
    up_matrix,
    up_scale,
    down_matrix,
    down_scale,
    *,
    sizes,
):
    count = sizes["fs"]
    order = ring_order(count)
    onward = [(order[i], order[(i + 1) % count]) for i in range(count)]
    spot = {device: i for i, device in enumerate(order)}
    table = [[order[(spot[device] - step) % count] for step in range(count)] for device in range(count)]
    half = lax.axis_index("rep")
    core = (lax.axis_index("tp") % 2).reshape(1)
    sources = jnp.asarray(table, jnp.int32)[lax.axis_index("fs")]
    places = jnp.stack([2 * sources + half, 2 * sources + 1 - half], axis=-1).reshape(-1)
    cores = [(i, i ^ 1) for i in range(sizes["tp"])]
    across = [(i, i ^ 2) for i in range(sizes["tp"])]
    flip = [(0, 1), (1, 0)]

    def halves(matrix):
        rows = matrix.shape[0] // 2
        near = lax.dynamic_slice_in_dim(matrix, half * rows, rows, 0).astype(jnp.bfloat16)
        far = lax.dynamic_slice_in_dim(matrix, (1 - half) * rows, rows, 0).astype(jnp.bfloat16)
        return near, far

    def shift(name, step, values):
        with jax.named_scope(f"z_{name}{step}"):
            return lax.ppermute(values, "fs", onward)

    def swap(name, step, values):
        with jax.named_scope(f"y_{name}{step}"):
            return lax.ppermute(values, "rep", flip)

    stream = tokens.reshape(tokens.shape[1], tokens.shape[2])
    chunk = stream.shape[1] // (2 * count)
    matrices = {"in": in_matrix, "out": out_matrix, "up": up_matrix, "down": down_matrix}
    pieces, moving = {}, {}
    for name, matrix in matrices.items():
        near, far = halves(matrix)
        pieces[name] = [near, far]
        moving[name] = near
    factors = jnp.stack([out_scale, down_scale]).astype(jnp.bfloat16)
    extra = jnp.pad(factors, ((0, 14), (0, 0)))
    moving["out"] = jnp.concatenate([moving["out"], extra], axis=0)
    factor_rows = [factors]
    turns = ["in1", "out1", "in2", "out2", "in3", "up1", "out3", "up2", "down1", "up3", "down2", "down3"]
    for turn in turns:
        name, step = turn[:-1], int(turn[-1])
        moving[name] = shift(name, step, moving[name])
        other = swap(name, step, moving[name])
        pieces[name] += [moving[name], other]
        if name == "out":
            factor_rows.append(moving[name][chunk : chunk + 2])
    stacked = jnp.stack(factor_rows, axis=1).reshape(2, count, 2, chunk).astype(jnp.float32)
    stacked = jnp.where(half == 0, stacked, stacked[:, :, ::-1])
    out_factor = stacked[0].reshape(1, -1)
    down_factor = stacked[1].reshape(count, 2, chunk)
    down_factor = jnp.where(core == 0, down_factor[:, 0], down_factor[:, 1])

    normed, stream = reorder(places, stream, first_gain, chunk)
    mixed = mixer(normed, pieces["in"], in_scale, conv_taps, decay_rate, recall_maps, admit_maps)
    kept, sent = project(core, mixed, pieces["out"], chunk)

    def add(one, two):
        return one.astype(jnp.float32) + two.astype(jnp.float32)

    def exchange(name, values, pairs):
        with jax.named_scope(name):
            return lax.ppermute(values, "tp", pairs)

    kept = add(kept, exchange("a_mix", sent, cores)).astype(jnp.bfloat16)
    own_mix = add(kept, exchange("b_mix", kept, across)).astype(jnp.bfloat16)
    peer_mix = exchange("c_mix", own_mix, cores)
    active, middle = expand(
        places, core, stream, own_mix, peer_mix, out_factor, second_gain, up_scale, pieces["up"]
    )
    own, peer = [], []
    for block in range(count):
        kept, sent = project(core, active, pieces["down"][2 * block : 2 * block + 2], chunk)
        kept = add(kept, exchange(f"a_down{block}", sent, cores)).astype(jnp.bfloat16)
        down = add(kept, exchange(f"b_down{block}", kept, across))
        result = middle[:, block * chunk : (block + 1) * chunk] + down_factor[block : block + 1] * down
        own.append(result.astype(jnp.bfloat16))
        peer.append(exchange(f"c_down{block}", own[-1], cores))
    return place(places, core, own, peer).reshape(tokens.shape)


def chosen_body(mesh):
    sizes = dict(mesh.shape)
    if sizes["rep"] == 2 and sizes["fs"] == 4 and sizes["tp"] == 4:
        return partial(ring_body, sizes=sizes)
    return plain_body


def solution(mesh):
    placed = (
        P(("rep", "fs"), None, None),
        P(),
        P("fs", "tp"),
        P("tp"),
        P(None, "tp"),
        P(None, "tp"),
        P(None, "tp", None, None),
        P(None, "tp", None, None),
        P("fs", "tp"),
        P("fs"),
        P(),
        P("fs", "tp"),
        P("tp"),
        P("fs", "tp"),
        P("fs"),
    )
    return jax.shard_map(
        chosen_body(mesh), mesh=mesh, in_specs=placed, out_specs=P(("rep", "fs"), None, None), check_vma=False
    )
```
